32 devices in a mesh: grp: 2 (over y), kv: 4 (over z), tp: 4 (over x, core).
Axes of the slice: x: 2, y: 2, z: 4, core: 2. Of those that a mesh axis runs over, the one named last changes fastest.
Arguments:
- candidate_embeddings: bfloat16 [1536, 4096], P(('grp', 'kv'), 'tp'), parts along dimension 0, may hold values from -100 to 100
- incoming_rms_scaling: float32 [4096], replicated, may hold values from 0.1 to 1.9
- probe_projector: bfloat16 [4096, 2048], P('kv', 'tp'), may hold values from -0.09375 to 0.09375
- address_projector: bfloat16 [4096, 2048], P('kv', 'tp'), may hold values from -0.09375 to 0.09375
- content_projector: bfloat16 [4096, 2048], P('kv', 'tp'), may hold values from -0.09375 to 0.09375
- sigmoid_mask_matrix: bfloat16 [4096, 2048], P('kv', 'tp'), may hold values from -0.09375 to 0.09375
- forgetting_projector: bfloat16 [4096, 16], replicated, may hold values from -0.09375 to 0.09375
- strength_projector_matrix: bfloat16 [4096, 16], replicated, may hold values from -0.09375 to 0.09375
- channel_forgetting_rates: float32 [16], P('tp'), may hold values from -3 to 0.5
- forgetting_offset: float32 [16], P('tp'), may hold values from -1 to 1
- extra_forgetting: float32 [384, 4, 16], P(('grp', 'kv'), None, 'tp'), parts along dimension 0, may hold values from -0.7 to 0, as said below
- outgoing_rms_scaling: float32 [128], replicated, may hold values from 0.1 to 1.9
- final_projector: bfloat16 [2048, 4096], P('tp', 'kv'), may hold values from -0.125 to 0.125
- memory_matrix: float32 [384, 16, 128, 128], P(('grp', 'kv'), 'tp'), parts along dimension 0, may hold values from -4 to 4
- earlier_addresses: bfloat16 [384, 4, 16, 128], P(('grp', 'kv'), None, 'tp'), parts along dimension 0, may hold values from -6 to 6
- earlier_contents: bfloat16 [384, 4, 16, 128], P(('grp', 'kv'), None, 'tp'), parts along dimension 0, may hold values from -6 to 6
- earlier_strengths: float32 [384, 4, 16], P(('grp', 'kv'), None, 'tp'), parts along dimension 0, may hold values from 0.1 to 0.9
- earlier_forgetting: float32 [384, 4, 16], P(('grp', 'kv'), None, 'tp'), parts along dimension 0, may hold values from -1.5 to -0.02
- admitted_counts: int32 [384], P(('grp', 'kv')), parts along dimension 0, may hold values from 0 to 4
Outputs:
- mixed: bfloat16 [1536, 4096], P(('grp', 'kv'), 'tp'), parts along dimension 0
- taken_state: float32 [384, 16, 128, 128], P(('grp', 'kv'), 'tp'), parts along dimension 0
The draws below stay inside these ranges and needn't reach their ends.
There are 2 independent parts, one for each index of `grp`. The reference program is written for one: setup_inputs(seed, part) draws one part's arguments, and reference() takes and returns one part's arrays. A program takes and returns all parts, laid end to end along the dimension named above; an argument that names none is the same for every part. Nothing has to cross between parts.
Inputs may be any that keep to these rules, and one draw needn't show every extreme that they name: `extra_forgetting`: mostly zero; elsewhere the logarithm of a factor between 0.5 and 0.8.
All inputs are finite; a program needn't handle non-finite values.
Results may differ from the reference program's by a relative error of at most 0.015.
Values may be sent and summed in bfloat16 or wider, within the bound.
No kernel may reach another device: no remote copies, remote signals or barrier semaphores. Data moves between devices by JAX's collectives and lax.ppermute only.
A program may use at most 128 MiB of HBM per device.

```python
import math
import jax
import jax.numpy as jnp
from jax import lax

D = 4096
H = 16
DK = 128
P_SIZE = 4
SEQS = 192
ROWS = 768
N_TP = 4


def draw_candidate_embeddings(key, part):
    key = jax.random.fold_in(key, 11)
    key_base, key_rows = jax.random.split(key)
    values_raw = jax.random.truncated_normal(key_base, -4.0, 4.0, (ROWS, D), jnp.float32)
    column = jnp.exp(math.log(10.0) * jnp.arange(D, dtype=jnp.float32) / D)
    row_scale = jnp.exp(jax.random.uniform(key_rows, (ROWS, 1), jnp.float32, 0.0, math.log(10.0)))
    return (values_raw * column[None, :] * row_scale / 4.0).astype(jnp.bfloat16)


def draw_extra_forgetting(key, part):
    key = jax.random.fold_in(key, 23)
    key_where, key_size = jax.random.split(key)
    struck = jax.random.randint(key_where, (SEQS, P_SIZE, H), 0, 8) == 0
    strength = jnp.log(jax.random.uniform(key_size, (SEQS, P_SIZE, H), jnp.float32, 0.5, 0.8))
    return jnp.where(struck, strength, jnp.zeros((SEQS, P_SIZE, H), jnp.float32))


def draw_admitted_counts(key, part):
    key = jax.random.fold_in(key, 37)
    return jax.random.randint(key, (SEQS,), 0, P_SIZE + 1).astype(jnp.int32)


def level_of(own_key, shape, pieces, low, largest):
    level, own = 1.0, jax.random.fold_in(own_key, 6)
    for position, shards_of in pieces:
        draws = jnp.exp(jax.random.uniform(jax.random.fold_in(own, position), (shards_of,), jnp.float32, low / len(pieces), largest / len(pieces)))
        level = level * jnp.repeat(draws, shape[position] // shards_of).reshape([-1 if axis == position else 1 for axis in range(len(shape))])
    return level


def noise(own_key, extent, scale, bound, pieces=(), kind=jnp.bfloat16):
    result = scale * jax.random.normal(own_key, extent, jnp.float32)
    if pieces:
        result = result * level_of(own_key, extent, pieces, -0.22, 0.18)
    return jnp.clip(result, -bound, bound).astype(kind)


def setup_inputs(seed: int = 0, part: int = 0) -> dict:
    seeds = jax.random.split(jax.random.key(seed), 20)
    own_keys = jax.random.split(jax.random.fold_in(seeds[19], part), 20)
    candidate_embeddings = draw_candidate_embeddings(jax.random.fold_in(jax.random.fold_in(seeds[19], part), 71), part)
    incoming_rms_scaling = jnp.clip(1.0 + 0.18 * jax.random.normal(seeds[1], (D,), jnp.float32), 0.1, 1.9)
    probe_projector = noise(seeds[2], (D, H * DK), D ** -0.5, 0.09375, ((0, 4), (1, 4)))
    address_projector = noise(seeds[3], (D, H * DK), D ** -0.5, 0.09375, ((0, 4), (1, 4)))
    content_projector = noise(seeds[4], (D, H * DK), D ** -0.5, 0.09375, ((0, 4), (1, 4)))
    sigmoid_mask_matrix = noise(seeds[5], (D, H * DK), D ** -0.5, 0.09375, ((0, 4), (1, 4)))
    forgetting_projector = noise(seeds[6], (D, H), D ** -0.5, 0.09375)
    strength_projector_matrix = noise(seeds[7], (D, H), D ** -0.5, 0.09375)
    channel_forgetting_rates = jnp.clip(-3.0 + 3.5 * jax.random.uniform(seeds[8], (H,), jnp.float32) ** level_of(seeds[8], (H,), ((0, 4),), -0.2, 0.2), -3.0, 0.5)
    forgetting_offset = jnp.clip(jax.random.uniform(seeds[9], (H,), jnp.float32, -1.0, 1.0) * level_of(seeds[9], (H,), ((0, 4),), -0.4, 0.0), -1.0, 1.0)
    extra_forgetting = draw_extra_forgetting(jax.random.fold_in(jax.random.fold_in(seeds[19], part), 71), part)
    outgoing_rms_scaling = jnp.clip(1.0 + 0.18 * jax.random.normal(seeds[11], (DK,), jnp.float32), 0.1, 1.9)
    final_projector = noise(seeds[12], (H * DK, D), (H * DK) ** -0.5, 0.125, ((0, 4), (1, 4)))
    memory_matrix = noise(own_keys[13], (SEQS, H, DK, DK), 0.25, 4.0, ((0, 4), (1, 4)), jnp.float32)
    earlier_addresses = noise(own_keys[14], (SEQS, P_SIZE, H, DK), 1.0, 6.0, ((0, 4), (2, 4)))
    earlier_contents = noise(own_keys[15], (SEQS, P_SIZE, H, DK), 1.0, 6.0, ((0, 4), (2, 4)))
    earlier_strengths = jnp.clip(0.1 + 0.79999997 * jax.random.uniform(own_keys[16], (SEQS, P_SIZE, H), jnp.float32) ** level_of(own_keys[16], (SEQS, P_SIZE, H), ((0, 4), (2, 4)), -0.2, 0.2), 0.1, 0.9)
    earlier_forgetting = jnp.clip(-1.5 + 1.48 * jax.random.uniform(own_keys[17], (SEQS, P_SIZE, H), jnp.float32) ** level_of(own_keys[17], (SEQS, P_SIZE, H), ((0, 4), (2, 4)), -0.2, 0.2), -1.5, -0.02)
    admitted_counts = draw_admitted_counts(jax.random.fold_in(jax.random.fold_in(seeds[19], part), 71), part)
    return {"candidate_embeddings": candidate_embeddings, "incoming_rms_scaling": incoming_rms_scaling, "probe_projector": probe_projector, "address_projector": address_projector, "content_projector": content_projector, "sigmoid_mask_matrix": sigmoid_mask_matrix, "forgetting_projector": forgetting_projector, "strength_projector_matrix": strength_projector_matrix, "channel_forgetting_rates": channel_forgetting_rates, "forgetting_offset": forgetting_offset, "extra_forgetting": extra_forgetting, "outgoing_rms_scaling": outgoing_rms_scaling, "final_projector": final_projector, "memory_matrix": memory_matrix, "earlier_addresses": earlier_addresses, "earlier_contents": earlier_contents, "earlier_strengths": earlier_strengths, "earlier_forgetting": earlier_forgetting, "admitted_counts": admitted_counts}


epsilon = 1e-06
highest = lax.Precision.HIGHEST

def unit_norm(vector):
    return vector * lax.rsqrt(lax.optimization_barrier(jnp.sum(vector * vector, axis=-1, keepdims=True)) + epsilon)

def update(carry, key_vec, value_vec, beta, log_decay):
    decayed = jnp.exp(log_decay)[..., None, None] * carry
    recalled = jnp.einsum('shde,shd->she', decayed, key_vec, precision=highest)
    return decayed + jnp.einsum('shd,she->shde', key_vec, beta[..., None] * (value_vec - recalled), precision=highest)

def stored(values):
    return lax.optimization_barrier(values.astype(jnp.bfloat16)).astype(jnp.float32)

def reference(candidate_embeddings, incoming_rms_scaling, probe_projector, address_projector, content_projector, sigmoid_mask_matrix, forgetting_projector, strength_projector_matrix, channel_forgetting_rates, forgetting_offset, extra_forgetting, outgoing_rms_scaling, final_projector, memory_matrix, earlier_addresses, earlier_contents, earlier_strengths, earlier_forgetting, admitted_counts):
    floated = candidate_embeddings.astype(jnp.float32)
    normed = (floated * lax.rsqrt(lax.optimization_barrier(jnp.mean(floated * floated, axis=1, keepdims=True)) + epsilon) * incoming_rms_scaling).astype(jnp.bfloat16)

    def project(weight):
        return stored(jnp.dot(normed, weight, preferred_element_type=jnp.float32)).reshape(SEQS, P_SIZE, H, DK)
    query = unit_norm(project(probe_projector)) * DK ** (-0.5)
    keyed = unit_norm(project(address_projector))
    valued = project(content_projector)
    gated = project(sigmoid_mask_matrix)
    forgetting_argument = jnp.dot(normed, forgetting_projector, preferred_element_type=jnp.float32).reshape(SEQS, P_SIZE, H)
    beta_in = jnp.dot(normed, strength_projector_matrix, preferred_element_type=jnp.float32).reshape(SEQS, P_SIZE, H)
    forgetting_multiplier = -jnp.exp(channel_forgetting_rates) * jax.nn.softplus(forgetting_argument + forgetting_offset) + extra_forgetting
    beta = jax.nn.sigmoid(beta_in)
    carried = memory_matrix
    for proposal in range(P_SIZE):
        fresh = update(carried, unit_norm(earlier_addresses[:, proposal].astype(jnp.float32)), earlier_contents[:, proposal].astype(jnp.float32), earlier_strengths[:, proposal], earlier_forgetting[:, proposal])
        live = (admitted_counts > proposal)[:, None, None, None]
        carried = jnp.where(live, fresh, carried)
    running = carried
    outputs = []
    for proposal in range(P_SIZE):
        running = update(running, keyed[:, proposal], valued[:, proposal], beta[:, proposal], forgetting_multiplier[:, proposal])
        outputs.append(jnp.einsum('shde,shd->she', running, query[:, proposal], precision=highest))
    attended = jnp.stack(outputs, axis=1)
    scaled = attended * lax.rsqrt(lax.optimization_barrier(jnp.mean(attended * attended, axis=-1, keepdims=True)) + epsilon) * outgoing_rms_scaling * jax.nn.silu(gated)
    flat = scaled.astype(jnp.bfloat16).reshape(ROWS, N_TP, H * DK // N_TP)
    weights = final_projector.reshape(N_TP, H * DK // N_TP, D)
    partial_value = jnp.einsum('rtc,tcd->rtd', flat.astype(jnp.float32), weights.astype(jnp.float32))
    mixed = lax.optimization_barrier(jnp.sum(stored(partial_value), axis=1)).astype(jnp.bfloat16)
    return (mixed, carried)
```

```python
import functools

import jax
import jax.numpy as jnp
from jax import lax
from jax.experimental import pallas as pl
from jax.experimental.pallas import tpu as pltpu
from jax.sharding import PartitionSpec as P

DK = 128
P_SIZE = 4
CORES = 2
CHUNKS = 2
BLOCK = 8
LANES = 32

epsilon = 1e-06
f32 = jnp.float32
bf16 = jnp.bfloat16


PAIRS = [(i, t) for t in range(P_SIZE) for i in range(t)]


def pair_lane(i, t):
    return 2 * P_SIZE + PAIRS.index((i, t))


def rows_of(outs, index):
    row = lax.broadcasted_iota(jnp.int32, (BLOCK, DK), 0)
    result = outs[0][index * BLOCK : (index + 1) * BLOCK]
    for s in range(1, BLOCK):
        result = jnp.where(row == s, outs[s][index * BLOCK : (index + 1) * BLOCK], result)
    return result


def split_two(values):
    high = values.astype(bf16)
    low = (values - high.astype(f32)).astype(bf16)
    return high, low


def state_products(vectors, state_ref, h):
    left = jnp.concatenate(vectors, axis=0).astype(bf16)
    left = jnp.concatenate([left, left], axis=1)
    outs = []
    for p in range(BLOCK // 2):
        both = jnp.concatenate([state_ref[2 * p, h], state_ref[2 * p + 1, h]], axis=1)
        high, low = split_two(both)
        out = jnp.dot(left, jnp.concatenate([high, low], axis=0), preferred_element_type=f32)
        outs += [out[:, :DK], out[:, DK:]]
    return outs


def row_dot(a, b):
    return jnp.sum(a * b, axis=1, keepdims=True)


def take_kernel(last_ref, coef_ref, key_ref, value_ref, state_ref, out_ref):
    heads = state_ref.shape[1]
    base = pl.program_id(0) * BLOCK
    coef = coef_ref[...]
    row_index = lax.broadcasted_iota(jnp.int32, (2 * P_SIZE * BLOCK, DK), 0) % BLOCK
    for h in range(heads):
        col = lambda p: coef[:, h * LANES + p : h * LANES + p + 1]
        keys = [key_ref[j, h] for j in range(P_SIZE)]
        outs = state_products(keys, state_ref, h)
        norms = [lax.rsqrt(row_dot(k, k) + epsilon) for k in keys]
        writes = []
        for j in range(P_SIZE):
            value = value_ref[j, h] - (col(P_SIZE + j) * norms[j]) * rows_of(outs, j)
            for i in range(j):
                factor = col(pair_lane(i, j)) * norms[i] * norms[j] * row_dot(keys[i], keys[j])
                value = value - factor * writes[i]
            writes.append(col(j) * value)
        ends = []
        for j in range(P_SIZE):
            factor = norms[j] if j == P_SIZE - 1 else norms[j] * col(pair_lane(j, P_SIZE - 1))
            ends.append(factor * writes[j])
        ends = jnp.concatenate(ends, axis=0)
        high = ends.astype(bf16).astype(f32)
        ends = jnp.concatenate([high, ends - high], axis=0)
        left = jnp.concatenate(keys + keys, axis=0).astype(bf16)
        for p in range(BLOCK // 2):
            masked = jnp.concatenate(
                [jnp.where(row_index == 2 * p + e, ends, 0.0) for e in range(2)], axis=1
            ).astype(bf16)
            added = lax.dot_general(
                left, masked, (((0,), (0,)), ((), ())), preferred_element_type=f32
            )
            for e in range(2):
                s = 2 * p + e
                out_ref[s, h] = (
                    last_ref[base + s, h] * state_ref[s, h] + added[:, e * DK : (e + 1) * DK]
                )


def take(memory, keys, values, coef, last):
    seqs, heads = memory.shape[:2]
    vector_spec = pl.BlockSpec((P_SIZE, heads, BLOCK, DK), lambda i: (0, 0, i, 0))
    state_spec = pl.BlockSpec((BLOCK, heads, DK, DK), lambda i: (i, 0, 0, 0))
    return pl.pallas_call(
        take_kernel,
        grid=(seqs // BLOCK,),
        in_specs=[
            pl.BlockSpec(memory_space=pltpu.SMEM),
            pl.BlockSpec((BLOCK, 128), lambda i: (i, 0)),
            vector_spec,
            vector_spec,
            state_spec,
        ],
        out_specs=state_spec,
        out_shape=jax.ShapeDtypeStruct(memory.shape, f32),
        cost_estimate=pl.CostEstimate(
            flops=memory.size * 64, bytes_accessed=memory.size * 8, transcendentals=0
        ),
        name="take",
    )(last, coef, keys, values, memory)


def read_kernel(coef_ref, scale_ref, gain_ref, a_ref, b_ref, c_ref, state_ref, out_ref, acc, flat):
    heads = state_ref.shape[1]
    coef = coef_ref[...]
    scale = scale_ref[...]
    gain = gain_ref[...]
    for block in range(4 * heads):
        at = pl.ds(block * DK, DK)
        total = a_ref[:, at].astype(f32) + b_ref[:, at].astype(f32) + c_ref[:, at].astype(f32)
        acc[block] = (total * scale).astype(bf16).astype(f32)
    for h in range(heads):
        col = lambda p: coef[:, h * LANES + p : h * LANES + p + 1]
        queries, keys, values, gates = [
            [acc[kind * heads + h, pl.ds(t, BLOCK, stride=P_SIZE), :] for t in range(P_SIZE)]
            for kind in range(4)
        ]
        outs = state_products(keys + queries, state_ref, h)
        norms = [lax.rsqrt(row_dot(k, k) + epsilon) for k in keys]
        writes = []
        for t in range(P_SIZE):
            value = values[t] - (col(P_SIZE + t) * norms[t]) * rows_of(outs, t)
            for i in range(t):
                factor = col(pair_lane(i, t)) * norms[i] * norms[t] * row_dot(keys[i], keys[t])
                value = value - factor * writes[i]
            writes.append(col(t) * value)
            query = queries[t]
            found = col(P_SIZE + t) * rows_of(outs, P_SIZE + t)
            for i in range(t + 1):
                factor = norms[i] * row_dot(keys[i], query)
                if i < t:
                    factor = factor * col(pair_lane(i, t))
                found = found + factor * writes[i]
            attended = found * (lax.rsqrt(row_dot(query, query) + epsilon) * DK ** (-0.5))
            mean = jnp.mean(attended * attended, axis=1, keepdims=True)
            gate = gates[t]
            flat[h, pl.ds(t, BLOCK, stride=P_SIZE), :] = (
                attended * lax.rsqrt(mean + epsilon) * gain * (gate * jax.nn.sigmoid(gate))
            )
        out_ref[:, pl.ds(h * DK, DK)] = flat[h].astype(bf16)


def read(chunk, parts, state, coef, scale, gain):
    seqs, heads = state.shape[:2]
    rows = BLOCK * P_SIZE
    steps = seqs // BLOCK // CHUNKS
    start = chunk * steps
    part_spec = pl.BlockSpec((rows, 4 * heads * DK), lambda i: (i, 0))
    return pl.pallas_call(
        read_kernel,
        grid=(steps,),
        in_specs=[
            pl.BlockSpec((BLOCK, 128), lambda i: (start + i, 0)),
            pl.BlockSpec((rows, 128), lambda i: (start + i, 0)),
            pl.BlockSpec((1, DK), lambda i: (0, 0)),
            part_spec,
            part_spec,
            part_spec,
            pl.BlockSpec((BLOCK, heads, DK, DK), lambda i: (start + i, 0, 0, 0)),
        ],
        out_specs=pl.BlockSpec((rows, heads * DK), lambda i: (i, 0)),
        out_shape=jax.ShapeDtypeStruct((steps * rows, heads * DK), bf16),
        scratch_shapes=[
            pltpu.VMEM((4 * heads, rows, DK), f32),
            pltpu.VMEM((heads, rows, DK), f32),
        ],
        cost_estimate=pl.CostEstimate(
            flops=state.size * 64 // CHUNKS,
            bytes_accessed=state.size * 4 // CHUNKS,
            transcendentals=0,
        ),
        name="read",
    )(coef, scale, gain, *parts, state)


def mix_kernel(index_ref, flat_ref, other_flat_ref, weight_ref, other_weight_ref, out_ref):
    out_ref[...] = (
        jnp.dot(flat_ref[...], weight_ref[0], preferred_element_type=f32)
        + jnp.dot(other_flat_ref[...], other_weight_ref[0], preferred_element_type=f32)
    ).astype(bf16)


def mix(flat, weight, other_weight, index, plane):
    rows = flat.shape[0]
    half, cols = weight.shape[1:]
    blocks = index.shape[0]
    scalars = jnp.concatenate([index, plane[None]]).astype(jnp.int32)
    weight_spec = pl.BlockSpec((1, half, cols), lambda i, s: (s[i], 0, 0))
    return pl.pallas_call(
        mix_kernel,
        grid_spec=pltpu.PrefetchScalarGridSpec(
            num_scalar_prefetch=1,
            grid=(blocks,),
            in_specs=[
                pl.BlockSpec((rows, half), lambda i, s: (0, s[blocks])),
                pl.BlockSpec((rows, half), lambda i, s: (0, 1 - s[blocks])),
                weight_spec,
                weight_spec,
            ],
            out_specs=pl.BlockSpec((rows, cols), lambda i, s: (0, i)),
        ),
        out_shape=jax.ShapeDtypeStruct((rows, blocks * cols), bf16),
        cost_estimate=pl.CostEstimate(
            flops=4 * rows * half * cols * blocks,
            bytes_accessed=4 * half * cols * blocks,
            transcendentals=0,
        ),
        name="mix",
    )(scalars, flat, flat, weight, other_weight)


def coefficients(strengths, log_decay):
    total = jnp.cumsum(log_decay, axis=1)
    parts = [strengths[:, t] for t in range(P_SIZE)]
    parts += [jnp.exp(total[:, t]) for t in range(P_SIZE)]
    for i, t in PAIRS:
        parts.append(jnp.exp(sum(log_decay[:, m] for m in range(i + 1, t + 1))))
    table = jnp.stack(parts, axis=-1)
    seqs, heads, used = table.shape
    table = jnp.pad(table, ((0, 0), (0, 0), (0, LANES - used))).reshape(seqs, heads * LANES)
    return jnp.pad(table, ((0, 0), (0, 128 - heads * LANES)))


def on_device(
    sizes,
    candidate_embeddings,
    incoming_rms_scaling,
    probe_projector,
    address_projector,
    content_projector,
    sigmoid_mask_matrix,
    forgetting_projector,
    strength_projector_matrix,
    channel_forgetting_rates,
    forgetting_offset,
    extra_forgetting,
    outgoing_rms_scaling,
    final_projector,
    memory_matrix,
    earlier_addresses,
    earlier_contents,
    earlier_strengths,
    earlier_forgetting,
    admitted_counts,
):
    planes, n_kv, n_tp = sizes
    rows, local_cols = candidate_embeddings.shape
    width = probe_projector.shape[1]
    heads = width // DK
    all_heads = forgetting_projector.shape[1]
    model = local_cols * n_tp
    seqs = rows // P_SIZE
    per_tp = n_kv // n_tp
    kv_cols = model // n_kv
    z = lax.axis_index("kv")
    tp = lax.axis_index("tp")
    plane = lax.axis_index("grp")
    core = tp % CORES

    def swap(value, mask):
        return lax.ppermute(value, "tp", [(i, i ^ mask) for i in range(n_tp)])

    gain_part = lax.dynamic_slice_in_dim(incoming_rms_scaling, tp * local_cols, local_cols)
    floated = candidate_embeddings.astype(f32)
    gained = (floated * gain_part).astype(bf16)
    small = jnp.concatenate([forgetting_projector, strength_projector_matrix], axis=1)
    small = lax.dynamic_slice_in_dim(small, tp * local_cols, local_cols)
    sums = jnp.concatenate(
        [
            jnp.dot(gained, small, preferred_element_type=f32),
            jnp.sum(floated * floated, axis=1, keepdims=True),
        ],
        axis=1,
    )
    mask = 1
    while mask < n_tp:
        sums = sums + swap(sums, mask)
        mask *= 2

    joined = jnp.concatenate(
        [probe_projector, address_projector, content_projector, sigmoid_mask_matrix], axis=1
    )

    half = width // 2
    near = lax.dynamic_slice_in_dim(final_projector, plane * half, half)
    far = lax.dynamic_slice_in_dim(final_projector, (1 - plane) * half, half)
    rights, lefts = [near], [near]
    for i in range(1, n_kv):
        rights.append(lax.ppermute(rights[-1], "kv", [(j, j + 1) for j in range(i - 1, n_kv - 1)]))
        lefts.append(lax.ppermute(lefts[-1], "kv", [(j + 1, j) for j in range(0, n_kv - i)]))
    near_blocks, far_blocks = [near], [far]
    for k in range(1, n_kv):
        block = jnp.where(z >= k, rights[k], lefts[n_kv - k])
        near_blocks.append(block)
        far_blocks.append(lax.ppermute(block, "grp", [(0, 1), (1, 0)]))
    near_weight = jnp.stack(near_blocks)
    far_weight = jnp.stack(far_blocks)

    live = admitted_counts[:, None, None] > jnp.arange(P_SIZE)[None, :, None]
    early_decay = jnp.where(live, earlier_forgetting, 0.0)
    early_coef = coefficients(jnp.where(live, earlier_strengths, 0.0), early_decay)
    by_head = lambda values: jnp.transpose(values, (1, 2, 0, 3)).astype(f32)
    taken = take(
        memory_matrix,
        by_head(earlier_addresses),
        by_head(earlier_contents),
        early_coef,
        jnp.exp(jnp.sum(early_decay, axis=1)),
    )

    scale = lax.rsqrt(sums[:, 2 * all_heads :] / model + epsilon)
    own = lambda at: lax.dynamic_slice_in_dim(sums, at + tp * heads, heads, 1) * scale
    decay_in = own(0).reshape(seqs, P_SIZE, heads)
    beta_in = own(all_heads).reshape(seqs, P_SIZE, heads)
    log_decay = (
        -jnp.exp(channel_forgetting_rates) * jax.nn.softplus(decay_in + forgetting_offset)
        + extra_forgetting
    )
    coef = coefficients(jax.nn.sigmoid(beta_in), log_decay)
    scale = jnp.broadcast_to(scale, (rows, 128))
    gain = outgoing_rms_scaling[None]

    chunk_rows = rows // CHUNKS
    part_rows = chunk_rows // CORES
    results = []
    for chunk in range(CHUNKS):
        first = chunk * chunk_rows
        halves = []
        for m in range(n_tp):
            at = first + part_rows * ((tp ^ m) % CORES)
            piece = lax.dynamic_slice_in_dim(gained, at, part_rows)
            halves.append(swap(piece, m) if m else piece)
        halves = jnp.stack(halves)

        def block_for(dest):
            return lax.dynamic_slice(
                halves,
                (tp ^ (dest // per_tp), 0, (dest % per_tp) * kv_cols),
                (1, part_rows, kv_cols),
            )[0]

        received = []
        for k in range(n_kv):
            piece = block_for((z + k) % n_kv)
            if k:
                piece = lax.ppermute(piece, "kv", [(i, (i + k) % n_kv) for i in range(n_kv)])
            received.append(piece)
        received = jnp.stack(received)
        partner = swap(received, 1)
        lower = jnp.where(core == 0, received, partner)
        upper = jnp.where(core == 0, partner, received)

        order = []
        for i in range(1, n_kv):
            order += [k for k in (i, n_kv - i) if k not in order]
        order.append(0)
        product = {}
        for k in order:
            block = jnp.concatenate([lower[k], upper[k]], axis=0)
            product[k] = jnp.dot(block, joined, preferred_element_type=f32)

        right = left = None
        for i in range(1, n_kv):
            send = product[i] if right is None else product[i] + right.astype(f32)
            right = lax.ppermute(send.astype(bf16), "kv", [(j, j + 1) for j in range(i)])
            send = product[n_kv - i] if left is None else product[n_kv - i] + left.astype(f32)
            left = lax.ppermute(
                send.astype(bf16), "kv", [(j, j - 1) for j in range(n_kv - i, n_kv)]
            )

        flat = read(
            chunk, (product[0].astype(bf16), right, left), taken, coef, scale, gain
        )

        def columns(masks):
            dest = jnp.concatenate(
                [(tp ^ m) * per_tp + jnp.arange(per_tp, dtype=jnp.int32) for m in masks]
            )
            return mix(flat, near_weight, far_weight, (z - dest) % n_kv, plane)

        away = swap(columns(range(1, n_tp, 2)), 1)
        home = columns(range(0, n_tp, 2)).astype(f32) + away.astype(f32)
        result = home[:, :local_cols]
        for m in range(1, n_tp // 2):
            piece = home[:, m * local_cols : (m + 1) * local_cols].astype(bf16)
            result = result + swap(piece, 2 * m).astype(f32)
        results.append(result.astype(bf16))
    return (jnp.concatenate(results, axis=0), taken)


def solution(mesh):
    in_specs = (
        P(("grp", "kv"), "tp"),
        P(),
        P("kv", "tp"),
        P("kv", "tp"),
        P("kv", "tp"),
        P("kv", "tp"),
        P(),
        P(),
        P("tp"),
        P("tp"),
        P(("grp", "kv"), None, "tp"),
        P(),
        P("tp", "kv"),
        P(("grp", "kv"), "tp", None, None),
        P(("grp", "kv"), None, "tp", None),
        P(("grp", "kv"), None, "tp", None),
        P(("grp", "kv"), None, "tp"),
        P(("grp", "kv"), None, "tp"),
        P(("grp", "kv")),
    )
    out_specs = (P(("grp", "kv"), "tp"), P(("grp", "kv"), "tp", None, None))
    sizes = tuple(mesh.shape[name] for name in ("grp", "kv", "tp"))
    return jax.shard_map(
        functools.partial(on_device, sizes),
        mesh=mesh,
        in_specs=in_specs,
        out_specs=out_specs,
        check_vma=False,
    )
```

```python
import functools

import jax
import jax.numpy as jnp
from jax import lax
from jax.experimental import pallas as pl
from jax.experimental.pallas import tpu as pltpu
from jax.sharding import PartitionSpec as P

DK = 128
P_SIZE = 4
CORES = 2
CHUNKS = 2
BLOCK = 8

epsilon = 1e-06
f32 = jnp.float32
bf16 = jnp.bfloat16


def rows_of(outs, index):
    row = lax.broadcasted_iota(jnp.int32, (BLOCK, DK), 0)
    result = outs[0][index * BLOCK : (index + 1) * BLOCK]
    for s in range(1, BLOCK):
        result = jnp.where(row == s, outs[s][index * BLOCK : (index + 1) * BLOCK], result)
    return result


def split_two(values):
    high = values.astype(bf16)
    low = (values - high.astype(f32)).astype(bf16)
    return high, low


def state_products(vectors, state_ref, h):
    left = jnp.concatenate(vectors, axis=0).astype(bf16)
    left = jnp.concatenate([left, left], axis=1)
    outs = []
    for p in range(BLOCK // 2):
        both = jnp.concatenate([state_ref[2 * p, h], state_ref[2 * p + 1, h]], axis=1)
        high, low = split_two(both)
        out = jnp.dot(left, jnp.concatenate([high, low], axis=0), preferred_element_type=f32)
        outs += [out[:, :DK], out[:, DK:]]
    return outs


def row_dot(a, b):
    return jnp.sum(a * b, axis=1, keepdims=True)


def decay_tables(log_decays):
    total = log_decays[0]
    starts = [jnp.exp(total)]
    for t in range(1, P_SIZE):
        total = total + log_decays[t]
        starts.append(jnp.exp(total))
    between = {}
    for i in range(P_SIZE):
        total = None
        for t in range(i + 1, P_SIZE):
            total = log_decays[t] if total is None else total + log_decays[t]
            between[i, t] = jnp.exp(total)
    return starts, between


def take_kernel(last_ref, aux_ref, key_ref, value_ref, state_ref, out_ref):
    heads = state_ref.shape[1]
    base = pl.program_id(0) * BLOCK
    aux = [aux_ref[pl.ds(j, BLOCK, stride=P_SIZE), :] for j in range(P_SIZE)]
    starts, between = decay_tables(aux)
    row_index = lax.broadcasted_iota(jnp.int32, (2 * P_SIZE * BLOCK, DK), 0) % BLOCK
    for h in range(heads):
        col = lambda table, lane=h: table[:, lane : lane + 1]
        keys = [key_ref[j, h] for j in range(P_SIZE)]
        outs = state_products(keys, state_ref, h)
        norms = [lax.rsqrt(row_dot(k, k) + epsilon) for k in keys]
        writes = []
        for j in range(P_SIZE):
            value = value_ref[j, h] - (col(starts[j]) * norms[j]) * rows_of(outs, j)
            for i in range(j):
                factor = col(between[i, j]) * norms[i] * norms[j] * row_dot(keys[i], keys[j])
                value = value - factor * writes[i]
            writes.append(col(aux[j], heads + h) * value)
        ends = []
        for j in range(P_SIZE):
            factor = norms[j] if j == P_SIZE - 1 else norms[j] * col(between[j, P_SIZE - 1])
            ends.append(factor * writes[j])
        ends = jnp.concatenate(ends, axis=0)
        high = ends.astype(bf16).astype(f32)
        ends = jnp.concatenate([high, ends - high], axis=0)
        left = jnp.concatenate(keys + keys, axis=0).astype(bf16)
        for p in range(BLOCK // 2):
            masked = jnp.concatenate(
                [jnp.where(row_index == 2 * p + e, ends, 0.0) for e in range(2)], axis=1
            ).astype(bf16)
            added = lax.dot_general(
                left, masked, (((0,), (0,)), ((), ())), preferred_element_type=f32
            )
            for e in range(2):
                s = 2 * p + e
                out_ref[s, h] = (
                    last_ref[base + s, h] * state_ref[s, h] + added[:, e * DK : (e + 1) * DK]
                )


def take(memory, keys, values, aux, last):
    seqs, heads = memory.shape[:2]
    vector_spec = pl.BlockSpec((P_SIZE, heads, BLOCK, DK), lambda i: (0, 0, i, 0))
    state_spec = pl.BlockSpec((BLOCK, heads, DK, DK), lambda i: (i, 0, 0, 0))
    return pl.pallas_call(
        take_kernel,
        grid=(seqs // BLOCK,),
        in_specs=[
            pl.BlockSpec(memory_space=pltpu.SMEM),
            pl.BlockSpec((BLOCK * P_SIZE, 128), lambda i: (i, 0)),
            vector_spec,
            vector_spec,
            state_spec,
        ],
        out_specs=state_spec,
        out_shape=jax.ShapeDtypeStruct(memory.shape, f32),
        cost_estimate=pl.CostEstimate(
            flops=memory.size * 64, bytes_accessed=memory.size * 8, transcendentals=0
        ),
        name="take",
    )(last, aux, keys, values, memory)


def read_kernel(
    aux_ref, gain_ref, own_ref, right_ref, left_ref, state_ref, out_ref, acc, vectors, found_ref, flat
):
    heads = state_ref.shape[1]
    step = pl.program_id(0)
    seqs = vectors.shape[2]
    rows = BLOCK * P_SIZE
    scale = aux_ref[pl.ds(step * rows, rows), :][:, 2 * heads : 2 * heads + 1]
    here = pl.ds(step * BLOCK, BLOCK)
    for kind in range(4):
        for h in range(heads):
            at = pl.ds((kind * heads + h) * DK, DK)
            total = own_ref[:, at] + right_ref[:, at].astype(f32) + left_ref[:, at].astype(f32)
            acc[kind * heads + h] = (total * scale).astype(bf16).astype(f32)
    for h in range(heads):
        picked = [
            acc[kind * heads + h, pl.ds(t, BLOCK, stride=P_SIZE), :]
            for kind in range(4)
            for t in range(P_SIZE)
        ]
        for n, value in enumerate(picked):
            vectors[n, h, here, :] = value
        outs = state_products(picked[: 2 * P_SIZE], state_ref, h)
        for n in range(2 * P_SIZE):
            found_ref[n, h, here, :] = rows_of(outs, n)

    @pl.when(step == pl.num_programs(0) - 1)
    def _():
        def whole(ref, n):
            return ref[n].reshape(heads * seqs, DK)

        def spread(table, first=0):
            return jnp.concatenate(
                [
                    jnp.broadcast_to(table[:, first + h : first + h + 1], (seqs, DK))
                    for h in range(heads)
                ],
                axis=0,
            )

        aux = [aux_ref[pl.ds(t, seqs, stride=P_SIZE), :] for t in range(P_SIZE)]
        starts, between = decay_tables(aux)
        gain = gain_ref[...]
        queries = [whole(vectors, t) for t in range(P_SIZE)]
        keys = [whole(vectors, P_SIZE + t) for t in range(P_SIZE)]
        norms = [lax.rsqrt(row_dot(k, k) + epsilon) for k in keys]
        writes = []
        for t in range(P_SIZE):
            start = spread(starts[t])
            steps = {i: spread(between[i, t]) for i in range(t)}
            value = whole(vectors, 2 * P_SIZE + t) - start * norms[t] * whole(found_ref, P_SIZE + t)
            for i in range(t):
                factor = steps[i] * (norms[i] * norms[t] * row_dot(keys[i], keys[t]))
                value = value - factor * writes[i]
            writes.append(spread(aux[t], heads) * value)
            query = queries[t]
            found = start * whole(found_ref, t)
            for i in range(t + 1):
                factor = norms[i] * row_dot(keys[i], query)
                if i < t:
                    factor = factor * steps[i]
                found = found + factor * writes[i]
            attended = found * (lax.rsqrt(row_dot(query, query) + epsilon) * DK ** (-0.5))
            mean = jnp.mean(attended * attended, axis=1, keepdims=True)
            gate = whole(vectors, 3 * P_SIZE + t)
            scaled = attended * lax.rsqrt(mean + epsilon) * gain * (gate * jax.nn.sigmoid(gate))
            for h in range(heads):
                flat[h, pl.ds(t, seqs, stride=P_SIZE), :] = scaled[h * seqs : (h + 1) * seqs]
        for h in range(heads):
            out_ref[:, pl.ds(h * DK, DK)] = flat[h].astype(bf16)


def read(chunk, own, right, left, state, aux, gain):
    seqs, heads = state.shape[:2]
    rows = BLOCK * P_SIZE
    steps = seqs // BLOCK // CHUNKS
    start = chunk * steps
    part_spec = pl.BlockSpec((rows, 4 * heads * DK), lambda i: (i, 0))
    return pl.pallas_call(
        read_kernel,
        grid=(steps,),
        in_specs=[
            pl.BlockSpec((steps * rows, 128), lambda i: (chunk, 0)),
            pl.BlockSpec((1, DK), lambda i: (0, 0)),
            part_spec,
            part_spec,
            part_spec,
            pl.BlockSpec((BLOCK, heads, DK, DK), lambda i: (start + i, 0, 0, 0)),
        ],
        out_specs=pl.BlockSpec((steps * rows, heads * DK), lambda i: (0, 0)),
        out_shape=jax.ShapeDtypeStruct((steps * rows, heads * DK), bf16),
        scratch_shapes=[
            pltpu.VMEM((4 * heads, rows, DK), f32),
            pltpu.VMEM((4 * P_SIZE, heads, steps * BLOCK, DK), f32),
            pltpu.VMEM((2 * P_SIZE, heads, steps * BLOCK, DK), f32),
            pltpu.VMEM((heads, steps * rows, DK), f32),
        ],
        cost_estimate=pl.CostEstimate(
            flops=state.size * 64 // CHUNKS,
            bytes_accessed=state.size * 4 // CHUNKS,
            transcendentals=0,
        ),
        name="read",
    )(aux, gain, own, right, left, state)


def mix_kernel(
    index_ref, flat_ref, other_flat_ref, weight_ref, other_weight_ref, away_ref, home_ref
):
    result = (
        jnp.dot(flat_ref[...], weight_ref[0], preferred_element_type=f32)
        + jnp.dot(other_flat_ref[...], other_weight_ref[0], preferred_element_type=f32)
    ).astype(bf16)
    away = pl.program_id(0) < pl.num_programs(0) // 2

    @pl.when(away)
    def _():
        away_ref[...] = result

    @pl.when(jnp.logical_not(away))
    def _():
        home_ref[...] = result


def mix(flat, weight, other_weight, index, plane):
    rows = flat.shape[0]
    half, cols = weight.shape[1:]
    blocks = index.shape[0]
    side = blocks // 2
    scalars = jnp.concatenate([index, plane[None]]).astype(jnp.int32)
    weight_spec = pl.BlockSpec((1, half, cols), lambda i, s: (s[i], 0, 0))
    out = jax.ShapeDtypeStruct((rows, side * cols), bf16)
    return pl.pallas_call(
        mix_kernel,
        grid_spec=pltpu.PrefetchScalarGridSpec(
            num_scalar_prefetch=1,
            grid=(blocks,),
            in_specs=[
                pl.BlockSpec((rows, half), lambda i, s: (0, s[blocks])),
                pl.BlockSpec((rows, half), lambda i, s: (0, 1 - s[blocks])),
                weight_spec,
                weight_spec,
            ],
            out_specs=[
                pl.BlockSpec((rows, cols), lambda i, s: (0, jnp.minimum(i, side - 1))),
                pl.BlockSpec((rows, cols), lambda i, s: (0, jnp.maximum(i - side, 0))),
            ],
        ),
        out_shape=[out, out],
        cost_estimate=pl.CostEstimate(
            flops=4 * rows * half * cols * blocks,
            bytes_accessed=4 * half * cols * blocks,
            transcendentals=0,
        ),
        name="mix",
    )(scalars, flat, flat, weight, other_weight)


def after(value, *others):
    return lax.optimization_barrier((value, *others))[0]


def on_device(
    sizes,
    candidate_embeddings,
    incoming_rms_scaling,
    probe_projector,
    address_projector,
    content_projector,
    sigmoid_mask_matrix,
    forgetting_projector,
    strength_projector_matrix,
    channel_forgetting_rates,
    forgetting_offset,
    extra_forgetting,
    outgoing_rms_scaling,
    final_projector,
    memory_matrix,
    earlier_addresses,
    earlier_contents,
    earlier_strengths,
    earlier_forgetting,
    admitted_counts,
):
    planes, n_kv, n_tp = sizes
    rows, local_cols = candidate_embeddings.shape
    width = probe_projector.shape[1]
    heads = width // DK
    all_heads = forgetting_projector.shape[1]
    model = local_cols * n_tp
    seqs = rows // P_SIZE
    per_tp = n_kv // n_tp
    kv_cols = model // n_kv
    z = lax.axis_index("kv")
    tp = lax.axis_index("tp")
    plane = lax.axis_index("grp")
    core = tp % CORES

    def swap(value, mask):
        return lax.ppermute(value, "tp", [(i, i ^ mask) for i in range(n_tp)])

    chunk_rows = rows // CHUNKS
    part_rows = chunk_rows // CORES

    gain_part = lax.dynamic_slice_in_dim(incoming_rms_scaling, tp * local_cols, local_cols)
    gained = (candidate_embeddings.astype(f32) * gain_part).astype(bf16)
    halves = []
    for chunk in range(CHUNKS):
        pieces = []
        for m in range(n_tp):
            at = chunk * chunk_rows + part_rows * ((tp ^ m) % CORES)
            piece = lax.dynamic_slice_in_dim(gained, at, part_rows)
            pieces.append(swap(piece, m) if m else piece)
        halves.append(jnp.stack(pieces))

    half = width // 2
    near = lax.dynamic_slice_in_dim(final_projector, plane * half, half)
    far = lax.dynamic_slice_in_dim(final_projector, (1 - plane) * half, half)
    rights, lefts = [near], [near]

    def weight_round(i, *others):
        right, left = lax.optimization_barrier((rights[-1], lefts[-1], *others))[:2]
        rights.append(lax.ppermute(right, "kv", [(j, j + 1) for j in range(i - 1, n_kv - 1)]))
        lefts.append(lax.ppermute(left, "kv", [(j + 1, j) for j in range(0, n_kv - i)]))

    weight_round(1, gained)

    joined = jnp.concatenate(
        [probe_projector, address_projector, content_projector, sigmoid_mask_matrix], axis=1
    )

    products = []
    for chunk in range(CHUNKS):

        def block_for(dest):
            return lax.dynamic_slice(
                halves[chunk],
                (tp ^ (dest // per_tp), 0, (dest % per_tp) * kv_cols),
                (1, part_rows, kv_cols),
            )[0]

        received = []
        for k in range(n_kv):
            piece = block_for((z + k) % n_kv)
            if k:
                piece = lax.ppermute(piece, "kv", [(i, (i + k) % n_kv) for i in range(n_kv)])
            received.append(piece)
        received = jnp.stack(received)
        partner = swap(received, 1)
        lower = jnp.where(core == 0, received, partner)
        upper = jnp.where(core == 0, partner, received)
        product = {}
        for i in range(n_kv // 2, 0, -1):
            pair = sorted({i % n_kv, n_kv - i}) if i < n_kv // 2 or n_kv == 2 else [0, i]
            block = jnp.concatenate([part[k] for k in pair for part in (lower, upper)], axis=0)
            out = jnp.dot(block, joined, preferred_element_type=f32)
            out = lax.optimization_barrier(out)
            for n, k in enumerate(pair):
                product[k] = out[n * chunk_rows : (n + 1) * chunk_rows]
        products.append(product)

    early = halves[0]
    small = jnp.concatenate([forgetting_projector, strength_projector_matrix], axis=1)
    small = lax.dynamic_slice_in_dim(small, tp * local_cols, local_cols)
    tied, raw = lax.optimization_barrier((gained, candidate_embeddings, early))[:2]
    raw = raw.astype(f32)
    sums = jnp.concatenate(
        [
            jnp.dot(tied, small, preferred_element_type=f32),
            jnp.sum(raw * raw, axis=1, keepdims=True),
        ],
        axis=1,
    )
    mask = 1
    while mask < n_tp:
        sums = sums + swap(sums, mask)
        mask *= 2

    arrived = [None] * CHUNKS
    for i in range(1, n_kv):
        for chunk in range(CHUNKS):
            product = products[chunk]
            sends = [product[i], product[n_kv - i]]
            if arrived[chunk] is not None:
                sends = [a + b.astype(f32) for a, b in zip(sends, arrived[chunk])]
            right, left = lax.optimization_barrier(tuple(v.astype(bf16) for v in sends))
            arrived[chunk] = (
                lax.ppermute(right, "kv", [(j, j + 1) for j in range(i)]),
                lax.ppermute(left, "kv", [(j, j - 1) for j in range(n_kv - i, n_kv)]),
            )
        if i < n_kv - 1:
            weight_round(i + 1, right)

    live = admitted_counts[:, None, None] > jnp.arange(P_SIZE)[None, :, None]
    early_decay = jnp.where(live, earlier_forgetting, 0.0)
    early_aux = jnp.concatenate([early_decay, jnp.where(live, earlier_strengths, 0.0)], axis=2)
    early_aux = jnp.pad(early_aux.reshape(rows, 2 * heads), ((0, 0), (0, 128 - 2 * heads)))
    by_head = lambda values: jnp.transpose(values, (1, 2, 0, 3)).astype(f32)
    memory = after(memory_matrix, products[-1][0])
    taken = take(
        memory,
        by_head(earlier_addresses),
        by_head(earlier_contents),
        early_aux,
        jnp.exp(jnp.sum(early_decay, axis=1)),
    )

    scale = lax.rsqrt(sums[:, 2 * all_heads :] / model + epsilon)
    own = lambda at: lax.dynamic_slice_in_dim(sums, at + tp * heads, heads, 1) * scale
    log_decay = -jnp.exp(channel_forgetting_rates) * jax.nn.softplus(
        own(0) + forgetting_offset
    ) + extra_forgetting.reshape(rows, heads)
    aux = jnp.concatenate([log_decay, jax.nn.sigmoid(own(all_heads)), scale], axis=1)
    aux = jnp.pad(aux, ((0, 0), (0, 128 - aux.shape[1])))
    gain = outgoing_rms_scaling[None]

    near_blocks, far_blocks = [near], [far]
    for k in range(1, n_kv):
        block = jnp.where(z >= k, rights[k], lefts[n_kv - k])
        near_blocks.append(block)
        if planes == 2:
            far_blocks.append(lax.ppermute(block, "grp", [(0, 1), (1, 0)]))
    near_weight = jnp.stack(near_blocks)
    far_weight = jnp.stack(far_blocks)

    masks = [*range(1, n_tp, 2), *range(0, n_tp, 2)]
    dest = jnp.concatenate(
        [(tp ^ m) * per_tp + jnp.arange(per_tp, dtype=jnp.int32) for m in masks]
    )
    index = (z - dest) % n_kv
    results = []
    for chunk in range(CHUNKS):
        flat = read(chunk, products[chunk][0], *arrived[chunk], taken, aux, gain)
        away, home = mix(flat, near_weight, far_weight, index, plane)
        home = home.astype(f32) + swap(away, 1).astype(f32)
        result = home[:, :local_cols]
        for m in range(1, n_tp // 2):
            piece = home[:, m * local_cols : (m + 1) * local_cols].astype(bf16)
            result = result + swap(piece, 2 * m).astype(f32)
        results.append(result.astype(bf16))
    return (jnp.concatenate(results, axis=0), taken)


def solution(mesh):
    in_specs = (
        P(("grp", "kv"), "tp"),
        P(),
        P("kv", "tp"),
        P("kv", "tp"),
        P("kv", "tp"),
        P("kv", "tp"),
        P(),
        P(),
        P("tp"),
        P("tp"),
        P(("grp", "kv"), None, "tp"),
        P(),
        P("tp", "kv"),
        P(("grp", "kv"), "tp", None, None),
        P(("grp", "kv"), None, "tp", None),
        P(("grp", "kv"), None, "tp", None),
        P(("grp", "kv"), None, "tp"),
        P(("grp", "kv"), None, "tp"),
        P(("grp", "kv")),
    )
    out_specs = (P(("grp", "kv"), "tp"), P(("grp", "kv"), "tp", None, None))
    sizes = tuple(mesh.shape[name] for name in ("grp", "kv", "tp"))
    return jax.shard_map(
        functools.partial(on_device, sizes),
        mesh=mesh,
        in_specs=in_specs,
        out_specs=out_specs,
        check_vma=False,
    )
```

```python
import functools

import jax
import jax.numpy as jnp
from jax import lax
from jax.experimental import pallas as pl
from jax.experimental.pallas import tpu as pltpu
from jax.sharding import PartitionSpec as P


DK = 128
P_SIZE = 4
CORES = 2
CHUNKS = 1
PIECES = 3
ENDS = 2
VMEM_LIMIT = 50 * 2**20
BLOCK = 8

epsilon = 1e-06
f32 = jnp.float32
bf16 = jnp.bfloat16


def rows_of(outs, index):
    row = lax.broadcasted_iota(jnp.int32, (BLOCK, DK), 0)
    result = outs[0][index * BLOCK : (index + 1) * BLOCK]
    for s in range(1, BLOCK):
        result = jnp.where(row == s, outs[s][index * BLOCK : (index + 1) * BLOCK], result)
    return result


def split_two(values):
    high = values.astype(bf16)
    low = (values - high.astype(f32)).astype(bf16)
    return high, low


def state_products(vectors, state_ref, h):
    left = jnp.concatenate(vectors, axis=0).astype(bf16)
    if state_ref.dtype == f32:
        left = jnp.concatenate([left, left], axis=1)
    outs = []
    for p in range(BLOCK // 2):
        both = jnp.concatenate([state_ref[2 * p, h], state_ref[2 * p + 1, h]], axis=1)
        if state_ref.dtype == f32:
            both = jnp.concatenate(split_two(both), axis=0)
        out = jnp.dot(left, both, preferred_element_type=f32)
        outs += [out[:, :DK], out[:, DK:]]
    return outs


def row_dot(a, b):
    return jnp.sum(a * b, axis=1, keepdims=True)


def decay_tables(log_decays):
    total = log_decays[0]
    starts = [jnp.exp(total)]
    for t in range(1, P_SIZE):
        total = total + log_decays[t]
        starts.append(jnp.exp(total))
    between = {}
    for i in range(P_SIZE):
        total = None
        for t in range(i + 1, P_SIZE):
            total = log_decays[t] if total is None else total + log_decays[t]
            between[i, t] = jnp.exp(total)
    return starts, between


def take_kernel(start, last_ref, aux_ref, key_ref, value_ref, state_ref, *refs):
    out_ref, rounded_ref = refs[-2:]
    heads = state_ref.shape[1]
    base = (start + pl.program_id(0)) * BLOCK
    aux = [aux_ref[pl.ds(j, BLOCK, stride=P_SIZE), :] for j in range(P_SIZE)]
    starts, between = decay_tables(aux)
    row_index = lax.broadcasted_iota(jnp.int32, (2 * P_SIZE * BLOCK, DK), 0) % BLOCK
    for h in range(heads):
        col = lambda table, lane=h: table[:, lane : lane + 1]
        keys = [key_ref[j, h] for j in range(P_SIZE)]
        outs = state_products(keys, state_ref, h)
        norms = [lax.rsqrt(row_dot(k, k) + epsilon) for k in keys]
        writes = []
        for j in range(P_SIZE):
            value = value_ref[j, h] - (col(starts[j]) * norms[j]) * rows_of(outs, j)
            for i in range(j):
                factor = col(between[i, j]) * norms[i] * norms[j] * row_dot(keys[i], keys[j])
                value = value - factor * writes[i]
            writes.append(col(aux[j], heads + h) * value)
        ends = []
        for j in range(P_SIZE):
            factor = norms[j] if j == P_SIZE - 1 else norms[j] * col(between[j, P_SIZE - 1])
            ends.append(factor * writes[j])
        ends = jnp.concatenate(ends, axis=0)
        high = ends.astype(bf16).astype(f32)
        ends = jnp.concatenate([high, ends - high], axis=0)
        left = jnp.concatenate(keys + keys, axis=0).astype(bf16)
        for p in range(BLOCK // 2):
            masked = jnp.concatenate(
                [jnp.where(row_index == 2 * p + e, ends, 0.0) for e in range(2)], axis=1
            ).astype(bf16)
            added = lax.dot_general(
                left, masked, (((0,), (0,)), ((), ())), preferred_element_type=f32
            )
            for e in range(2):
                s = 2 * p + e
                taken = last_ref[base + s, h] * state_ref[s, h] + added[:, e * DK : (e + 1) * DK]
                out_ref[s, h] = taken
                rounded_ref[s, h] = taken.astype(bf16)


def take(piece, before, memory, keys, values, aux, last):
    seqs, heads = memory.shape[:2]
    steps = seqs // BLOCK // PIECES
    start = piece * steps
    vector_spec = pl.BlockSpec((P_SIZE, heads, BLOCK, DK), lambda i: (0, 0, start + i, 0))
    state_spec = pl.BlockSpec((BLOCK, heads, DK, DK), lambda i: (start + i, 0, 0, 0))
    in_specs = [
        pl.BlockSpec(memory_space=pltpu.SMEM),
        pl.BlockSpec((BLOCK * P_SIZE, 128), lambda i: (start + i, 0)),
        vector_spec,
        vector_spec,
        state_spec,
    ]
    operands = [last, aux, keys, values, memory]
    aliases = {}
    if before is not None:
        in_specs += [pl.BlockSpec(memory_space=pl.ANY)] * 2
        aliases = {len(operands): 0, len(operands) + 1: 1}
        operands += before
    return pl.pallas_call(
        functools.partial(take_kernel, start),
        grid=(steps,),
        in_specs=in_specs,
        out_specs=[state_spec, state_spec],
        out_shape=[jax.ShapeDtypeStruct(memory.shape, kind) for kind in (f32, bf16)],
        input_output_aliases=aliases,
        compiler_params=pltpu.CompilerParams(vmem_limit_bytes=VMEM_LIMIT),
        cost_estimate=pl.CostEstimate(
            flops=memory.size * 64 // PIECES,
            bytes_accessed=memory.size * 8 // PIECES,
            transcendentals=0,
        ),
        name="take",
    )(*operands)


def finish_kernel(n_refs, position_ref, aux_ref, gain_ref, own_ref, right_ref, left_ref, *refs):
    state_ref, *refs = refs
    near_refs, far_refs, refs = refs[:n_refs], refs[n_refs : 2 * n_refs], refs[2 * n_refs :]
    away_ref, home_ref, acc, vectors, found_ref, flat, weights, sems = refs
    heads = state_ref.shape[1]
    step = pl.program_id(0)
    seqs = vectors.shape[2]
    rows = BLOCK * P_SIZE
    n_blocks = weights.shape[0]

    def each_copy(act):
        for k in range(n_refs):

            @pl.when(position_ref[k] >= 0)
            def _():
                for side, refs in enumerate((near_refs, far_refs)):
                    into = weights.at[position_ref[k], side]
                    act(pltpu.make_async_copy(refs[k], into, sems.at[k, side]))

    @pl.when(step == 0)
    def _():
        each_copy(lambda copy: copy.start())

    scale = aux_ref[pl.ds(step * rows, rows), :][:, 2 * heads : 2 * heads + 1]
    here = pl.ds(step * BLOCK, BLOCK)
    for kind in range(4):
        for h in range(heads):
            at = pl.ds((kind * heads + h) * DK, DK)
            total = own_ref[:, at] + right_ref[:, at].astype(f32) + left_ref[:, at].astype(f32)
            acc[kind * heads + h] = (total * scale).astype(bf16).astype(f32)
    for h in range(heads):
        picked = [
            acc[kind * heads + h, pl.ds(t, BLOCK, stride=P_SIZE), :]
            for kind in range(4)
            for t in range(P_SIZE)
        ]
        for n, value in enumerate(picked):
            vectors[n, h, here, :] = value
        outs = state_products(picked[: 2 * P_SIZE], state_ref, h)
        for n in range(2 * P_SIZE):
            found_ref[n, h, here, :] = rows_of(outs, n)

    @pl.when(step == pl.num_programs(0) - 1)
    def _():
        def whole(ref, n):
            return ref[n].reshape(heads * seqs, DK)

        def spread(table, first=0):
            return jnp.concatenate(
                [
                    jnp.broadcast_to(table[:, first + h : first + h + 1], (seqs, DK))
                    for h in range(heads)
                ],
                axis=0,
            )

        aux = [aux_ref[pl.ds(t, seqs, stride=P_SIZE), :] for t in range(P_SIZE)]
        starts, between = decay_tables(aux)
        gain = gain_ref[...]
        queries = [whole(vectors, t) for t in range(P_SIZE)]
        keys = [whole(vectors, P_SIZE + t) for t in range(P_SIZE)]
        norms = [lax.rsqrt(row_dot(k, k) + epsilon) for k in keys]
        writes = []
        for t in range(P_SIZE):
            start = spread(starts[t])
            steps = {i: spread(between[i, t]) for i in range(t)}
            value = whole(vectors, 2 * P_SIZE + t) - start * norms[t] * whole(found_ref, P_SIZE + t)
            for i in range(t):
                factor = steps[i] * (norms[i] * norms[t] * row_dot(keys[i], keys[t]))
                value = value - factor * writes[i]
            writes.append(spread(aux[t], heads) * value)
            query = queries[t]
            found = start * whole(found_ref, t)
            for i in range(t + 1):
                factor = norms[i] * row_dot(keys[i], query)
                if i < t:
                    factor = factor * steps[i]
                found = found + factor * writes[i]
            attended = found * (lax.rsqrt(row_dot(query, query) + epsilon) * DK ** (-0.5))
            mean = jnp.mean(attended * attended, axis=1, keepdims=True)
            gate = whole(vectors, 3 * P_SIZE + t)
            scaled = attended * lax.rsqrt(mean + epsilon) * gain * (gate * jax.nn.sigmoid(gate))
            for h in range(heads):
                flat[h, pl.ds(t, seqs, stride=P_SIZE), :] = scaled[h * seqs : (h + 1) * seqs]
        sides = heads // 2
        plane = position_ref[n_refs]
        lefts = [
            jnp.concatenate([flat[first + h] for h in range(sides)], axis=1).astype(bf16)
            for first in (plane * sides, (1 - plane) * sides)
        ]
        each_copy(lambda copy: copy.wait())
        cols = weights.shape[-1]
        for n in range(n_blocks):
            result = sum(
                jnp.dot(lefts[side], weights[n, side], preferred_element_type=f32)
                for side in range(2)
            ).astype(bf16)
            out_ref, at = (away_ref, n) if n < n_blocks // 2 else (home_ref, n - n_blocks // 2)
            out_ref[:, pl.ds(at * cols, cols)] = result


def finish(chunk, n_blocks, own, right, left, state, aux, gain, near, far, position):
    seqs, heads = state.shape[:2]
    rows = BLOCK * P_SIZE
    steps = seqs // BLOCK // ENDS
    start = chunk * steps
    first = start % (own.shape[0] // rows)
    n_refs = len(near)
    half, cols = near[0].shape
    part_spec = lambda at: pl.BlockSpec((rows, 4 * heads * DK), lambda i: (at + i, 0))
    out = jax.ShapeDtypeStruct((steps * rows, n_blocks // 2 * cols), bf16)
    out_spec = pl.BlockSpec(out.shape, lambda i: (0, 0))
    return pl.pallas_call(
        functools.partial(finish_kernel, n_refs),
        grid=(steps,),
        in_specs=[
            pl.BlockSpec(memory_space=pltpu.SMEM),
            pl.BlockSpec((steps * rows, 128), lambda i: (chunk, 0)),
            pl.BlockSpec((1, DK), lambda i: (0, 0)),
            part_spec(first),
            part_spec(0),
            part_spec(0),
            pl.BlockSpec((BLOCK, heads, DK, DK), lambda i: (start + i, 0, 0, 0)),
            *[pl.BlockSpec(memory_space=pl.ANY)] * (2 * n_refs),
        ],
        out_specs=[out_spec, out_spec],
        out_shape=[out, out],
        scratch_shapes=[
            pltpu.VMEM((4 * heads, rows, DK), f32),
            pltpu.VMEM((4 * P_SIZE, heads, steps * BLOCK, DK), f32),
            pltpu.VMEM((2 * P_SIZE, heads, steps * BLOCK, DK), f32),
            pltpu.VMEM((heads, steps * rows, DK), f32),
            pltpu.VMEM((n_blocks, 2, half, cols), bf16),
            pltpu.SemaphoreType.DMA((n_refs, 2)),
        ],
        compiler_params=pltpu.CompilerParams(vmem_limit_bytes=VMEM_LIMIT),
        cost_estimate=pl.CostEstimate(
            flops=state.size * 64 // ENDS,
            bytes_accessed=state.size * 2 // ENDS,
            transcendentals=0,
        ),
        name="finish",
    )(position, aux, gain, own, right, left, state, *near, *far)


def after(value, *others):
    return lax.optimization_barrier((value, *others))[0]


def on_device(
    sizes,
    candidate_embeddings,
    incoming_rms_scaling,
    probe_projector,
    address_projector,
    content_projector,
    sigmoid_mask_matrix,
    forgetting_projector,
    strength_projector_matrix,
    channel_forgetting_rates,
    forgetting_offset,
    extra_forgetting,
    outgoing_rms_scaling,
    final_projector,
    memory_matrix,
    earlier_addresses,
    earlier_contents,
    earlier_strengths,
    earlier_forgetting,
    admitted_counts,
):
    _, n_kv, n_tp = sizes
    rows, local_cols = candidate_embeddings.shape
    width = probe_projector.shape[1]
    heads = width // DK
    all_heads = forgetting_projector.shape[1]
    model = local_cols * n_tp
    per_tp = n_kv // n_tp
    kv_cols = model // n_kv
    z = lax.axis_index("kv")
    tp = lax.axis_index("tp")
    plane = lax.axis_index("grp")
    core = tp % CORES

    def swap(value, mask):
        return lax.ppermute(value, "tp", [(i, i ^ mask) for i in range(n_tp)])

    chunk_rows = rows // CHUNKS
    part_rows = chunk_rows // CORES

    gain_part = lax.dynamic_slice_in_dim(incoming_rms_scaling, tp * local_cols, local_cols)
    gained = (candidate_embeddings.astype(f32) * gain_part).astype(bf16)
    halves = []
    for chunk in range(CHUNKS):
        pieces = []
        for m in range(n_tp):
            at = chunk * chunk_rows + part_rows * ((tp ^ m) % CORES)
            pieces.append(lax.dynamic_slice_in_dim(gained, at, part_rows))
        for m in range(n_tp - 1, 0, -1):
            pieces[m] = swap(pieces[m], m)
        halves.append(jnp.stack(pieces))

    half = width // 2
    near = lax.dynamic_slice_in_dim(final_projector, plane * half, half)
    far = lax.dynamic_slice_in_dim(final_projector, (1 - plane) * half, half)
    rights, lefts = [near], [near]
    far_rights, far_lefts = [far], [far]

    def weight_round(i, *others):
        right, left = lax.optimization_barrier((rights[-1], lefts[-1], *others))[:2]
        pairs = [(j, j + 1) for j in range(i - 1, n_kv - 1)]
        rights.append(lax.ppermute(right, "kv", pairs))
        pairs = [(j + 1, j) for j in range(0, n_kv - i)]
        lefts.append(lax.ppermute(left, "kv", pairs))

    def weight_cross(i):
        def pairs(places):
            return [(g * n_kv + j, (1 - g) * n_kv + j) for g in range(2) for j in places]

        both = ("grp", "kv")
        right, left = lax.optimization_barrier((rights[i], lefts[i]))
        far_rights.append(lax.ppermute(right, both, pairs(range(i, n_kv))))
        far_lefts.append(lax.ppermute(left, both, pairs(range(n_kv - i))))

    weight_round(1, gained)

    joined = jnp.concatenate(
        [probe_projector, address_projector, content_projector, sigmoid_mask_matrix], axis=1
    )

    received = []
    for chunk in range(CHUNKS):

        def block_for(dest):
            return lax.dynamic_slice(
                halves[chunk],
                (tp ^ (dest // per_tp), 0, (dest % per_tp) * kv_cols),
                (1, part_rows, kv_cols),
            )[0]

        sends = lax.optimization_barrier(tuple(block_for((z + k) % n_kv) for k in range(n_kv)))
        received.append(
            [sends[0]]
            + [
                lax.ppermute(sends[k], "kv", [(i, (i + k) % n_kv) for i in range(n_kv)])
                for k in range(1, n_kv)
            ]
        )

    blocks = [None] * CHUNKS
    products = [{} for _ in range(CHUNKS)]
    arrived = [None] * CHUNKS
    token = received[0][0]
    crossing = crossing_order(n_kv)
    for i in range(1, n_kv):
        for chunk in range(CHUNKS):
            product = products[chunk]
            if i == 1:
                mine = lax.optimization_barrier((*received[chunk], token))[:n_kv]
                blocks[chunk] = [None] * n_kv
                for k in crossing:
                    partner = swap(mine[k], 1)
                    blocks[chunk][k] = jnp.concatenate(
                        [
                            jnp.where(core == 0, mine[k], partner),
                            jnp.where(core == 0, partner, mine[k]),
                        ]
                    )
            if i <= n_kv // 2:
                pair = [i, n_kv - i] if i < n_kv - i else [0, i]
                block = jnp.concatenate([blocks[chunk][k] for k in pair], axis=0)
                block = after(block, token)
                out = jnp.dot(block, joined, preferred_element_type=f32)
                out = lax.optimization_barrier(out)
                for n, k in enumerate(pair):
                    product[k] = out[n * chunk_rows : (n + 1) * chunk_rows]
            sends = [product[i], product[n_kv - i]]
            places = (
                [(j, j + 1) for j in range(i)],
                [(j, j - 1) for j in range(n_kv - i, n_kv)],
            )
            parts = ENDS // CHUNKS if i == n_kv - 1 else 1
            part = chunk_rows // parts
            for side in range(2):
                if arrived[chunk] is not None:
                    there = after(arrived[chunk][0][side], token)
                    sends[side] = sends[side] + there.astype(f32)
                token = sends[side] = lax.optimization_barrier(sends[side].astype(bf16))
            got = []
            for n in range(parts):
                both = []
                for side in range(2):
                    send = sends[side]
                    if parts > 1:
                        send = lax.optimization_barrier(send[n * part : (n + 1) * part])
                    both.append(lax.ppermute(send, "kv", places[side]))
                got.append(tuple(both))
            arrived[chunk] = got
            if chunk == 0:
                if 2 * i < n_kv:
                    weight_round(2 * i, token)
                for q in range(max(2 * i - 2, 1), min(2 * i, n_kv)):
                    weight_cross(q)
                if 2 * i + 1 < n_kv:
                    weight_round(2 * i + 1, token)
        if i == 1:
            first_arrived = arrived[0][0][0]

    early = lax.optimization_barrier(
        (
            admitted_counts,
            earlier_forgetting,
            earlier_strengths,
            earlier_addresses,
            earlier_contents,
            gained,
        )
    )
    live = early[0][:, None, None] > jnp.arange(P_SIZE)[None, :, None]
    early_decay = jnp.where(live, early[1], 0.0)
    early_aux = jnp.concatenate([early_decay, jnp.where(live, early[2], 0.0)], axis=2)
    early_aux = jnp.pad(early_aux.reshape(rows, 2 * heads), ((0, 0), (0, 128 - 2 * heads)))
    by_head = lambda values: jnp.transpose(values, (1, 2, 0, 3)).astype(f32)
    early_keys, early_values = by_head(early[3]), by_head(early[4])
    early_last = jnp.exp(jnp.sum(early_decay, axis=1))
    taken = None
    for piece in range(PIECES):
        taken = take(piece, taken, memory_matrix, early_keys, early_values, early_aux, early_last)

    small = jnp.concatenate([forgetting_projector, strength_projector_matrix], axis=1)
    small = lax.dynamic_slice_in_dim(small, tp * local_cols, local_cols)
    tied, raw = lax.optimization_barrier((gained, candidate_embeddings, first_arrived))[:2]
    raw = raw.astype(f32)
    sums = jnp.concatenate(
        [
            jnp.dot(tied, small, preferred_element_type=f32),
            jnp.sum(raw * raw, axis=1, keepdims=True),
        ],
        axis=1,
    )
    mask = 1
    while mask < n_tp:
        sums = sums + lax.ppermute(sums, "tp", [(i, i ^ mask) for i in range(n_tp)])
        mask *= 2
    scale = lax.rsqrt(sums[:, 2 * all_heads :] / model + epsilon)
    own = lambda at: lax.dynamic_slice_in_dim(sums, at + tp * heads, heads, 1) * scale
    log_decay = -jnp.exp(channel_forgetting_rates) * jax.nn.softplus(
        own(0) + forgetting_offset
    ) + extra_forgetting.reshape(rows, heads)
    aux = jnp.concatenate([log_decay, jax.nn.sigmoid(own(all_heads)), scale], axis=1)
    aux = jnp.pad(aux, ((0, 0), (0, 128 - aux.shape[1])))
    gain = outgoing_rms_scaling[None]

    offsets = [0] + [-i for i in range(1, n_kv)] + list(range(1, n_kv))
    source = z + jnp.array(offsets, dtype=jnp.int32)
    apart = tp ^ (source // per_tp)
    position = (apart // 2 + jnp.where(apart % 2 == 0, n_tp // 2, 0)) * per_tp + source % per_tp
    position = jnp.where((source >= 0) & (source < n_kv), position, -1)
    position = jnp.concatenate([position, plane[None]]).astype(jnp.int32)
    results = []
    for end in range(ENDS):
        chunk = end * CHUNKS // ENDS
        away, home = finish(
            end,
            n_kv,
            products[chunk][0],
            *arrived[chunk][end % (ENDS // CHUNKS)],
            taken[1],
            aux,
            gain,
            rights + lefts[1:],
            far_rights + far_lefts[1:],
            position,
        )
        home = home.astype(f32) + swap(away, 1).astype(f32)
        result = home[:, :local_cols]
        for m in range(1, n_tp // 2):
            piece = home[:, m * local_cols : (m + 1) * local_cols].astype(bf16)
            result = result + swap(piece, 2 * m).astype(f32)
        results.append(result.astype(bf16))
    return (jnp.concatenate(results, axis=0), taken[0])


def crossing_order(n_kv):
    first = [k for i in range(1, (n_kv + 1) // 2) for k in (i, n_kv - i)]
    return first + [k for k in range(n_kv) if k not in first]


def solution(mesh):
    in_specs = (
        P(("grp", "kv"), "tp"),
        P(),
        P("kv", "tp"),
        P("kv", "tp"),
        P("kv", "tp"),
        P("kv", "tp"),
        P(),
        P(),
        P("tp"),
        P("tp"),
        P(("grp", "kv"), None, "tp"),
        P(),
        P("tp", "kv"),
        P(("grp", "kv"), "tp", None, None),
        P(("grp", "kv"), None, "tp", None),
        P(("grp", "kv"), None, "tp", None),
        P(("grp", "kv"), None, "tp"),
        P(("grp", "kv"), None, "tp"),
        P(("grp", "kv")),
    )
    out_specs = (P(("grp", "kv"), "tp"), P(("grp", "kv"), "tp", None, None))
    sizes = tuple(mesh.shape[name] for name in ("grp", "kv", "tp"))

    def layer(*arrays):
        return on_device(sizes, *arrays)

    return jax.shard_map(
        layer, mesh=mesh, in_specs=in_specs, out_specs=out_specs, check_vma=False
    )
```

```python
import functools

import jax
import jax.numpy as jnp
from jax import lax
from jax.experimental import pallas as pl
from jax.experimental.pallas import tpu as pltpu
from jax.sharding import PartitionSpec as P


DK = 128
P_SIZE = 4
CORES = 2
CHUNKS = 1
PIECES = 3
ENDS = 2
VMEM_LIMIT = 50 * 2**20
BLOCK = 8

epsilon = 1e-06
f32 = jnp.float32
bf16 = jnp.bfloat16


def rows_of(outs, index):
    row = lax.broadcasted_iota(jnp.int32, (BLOCK, DK), 0)
    result = outs[0][index * BLOCK : (index + 1) * BLOCK]
    for s in range(1, BLOCK):
        result = jnp.where(row == s, outs[s][index * BLOCK : (index + 1) * BLOCK], result)
    return result


def split_two(values):
    high = values.astype(bf16)
    low = (values - high.astype(f32)).astype(bf16)
    return high, low


def state_products(vectors, state_ref, h):
    left = jnp.concatenate(vectors, axis=0).astype(bf16)
    if state_ref.dtype == f32:
        left = jnp.concatenate([left, left], axis=1)
    outs = []
    for p in range(BLOCK // 2):
        both = jnp.concatenate([state_ref[2 * p, h], state_ref[2 * p + 1, h]], axis=1)
        if state_ref.dtype == f32:
            both = jnp.concatenate(split_two(both), axis=0)
        out = jnp.dot(left, both, preferred_element_type=f32)
        outs += [out[:, :DK], out[:, DK:]]
    return outs


def row_dot(a, b):
    return jnp.sum(a * b, axis=1, keepdims=True)


def decay_tables(log_decays):
    total = log_decays[0]
    starts = [jnp.exp(total)]
    for t in range(1, P_SIZE):
        total = total + log_decays[t]
        starts.append(jnp.exp(total))
    between = {}
    for i in range(P_SIZE):
        total = None
        for t in range(i + 1, P_SIZE):
            total = log_decays[t] if total is None else total + log_decays[t]
            between[i, t] = jnp.exp(total)
    return starts, between


def take_kernel(start, last_ref, aux_ref, key_ref, value_ref, state_ref, *refs):
    out_ref, rounded_ref = refs[-2:]
    heads = state_ref.shape[1]
    base = (start + pl.program_id(0)) * BLOCK
    aux = [aux_ref[pl.ds(j, BLOCK, stride=P_SIZE), :] for j in range(P_SIZE)]
    starts, between = decay_tables(aux)
    row_index = lax.broadcasted_iota(jnp.int32, (2 * P_SIZE * BLOCK, DK), 0) % BLOCK
    for h in range(heads):
        col = lambda table, lane=h: table[:, lane : lane + 1]
        keys = [key_ref[j, h] for j in range(P_SIZE)]
        outs = state_products(keys, state_ref, h)
        norms = [lax.rsqrt(row_dot(k, k) + epsilon) for k in keys]
        writes = []
        for j in range(P_SIZE):
            value = value_ref[j, h] - (col(starts[j]) * norms[j]) * rows_of(outs, j)
            for i in range(j):
                factor = col(between[i, j]) * norms[i] * norms[j] * row_dot(keys[i], keys[j])
                value = value - factor * writes[i]
            writes.append(col(aux[j], heads + h) * value)
        ends = []
        for j in range(P_SIZE):
            factor = norms[j] if j == P_SIZE - 1 else norms[j] * col(between[j, P_SIZE - 1])
            ends.append(factor * writes[j])
        ends = jnp.concatenate(ends, axis=0)
        high = ends.astype(bf16).astype(f32)
        ends = jnp.concatenate([high, ends - high], axis=0)
        left = jnp.concatenate(keys + keys, axis=0).astype(bf16)
        for p in range(BLOCK // 2):
            masked = jnp.concatenate(
                [jnp.where(row_index == 2 * p + e, ends, 0.0) for e in range(2)], axis=1
            ).astype(bf16)
            added = lax.dot_general(
                left, masked, (((0,), (0,)), ((), ())), preferred_element_type=f32
            )
            for e in range(2):
                s = 2 * p + e
                taken = last_ref[base + s, h] * state_ref[s, h] + added[:, e * DK : (e + 1) * DK]
                out_ref[s, h] = taken
                rounded_ref[s, h] = taken.astype(bf16)


def take(piece, before, memory, keys, values, aux, last):
    seqs, heads = memory.shape[:2]
    steps = seqs // BLOCK // PIECES
    start = piece * steps
    vector_spec = pl.BlockSpec((P_SIZE, heads, BLOCK, DK), lambda i: (0, 0, start + i, 0))
    state_spec = pl.BlockSpec((BLOCK, heads, DK, DK), lambda i: (start + i, 0, 0, 0))
    in_specs = [
        pl.BlockSpec(memory_space=pltpu.SMEM),
        pl.BlockSpec((BLOCK * P_SIZE, 128), lambda i: (start + i, 0)),
        vector_spec,
        vector_spec,
        state_spec,
    ]
    operands = [last, aux, keys, values, memory]
    aliases = {}
    if before is not None:
        in_specs += [pl.BlockSpec(memory_space=pl.ANY)] * 2
        aliases = {len(operands): 0, len(operands) + 1: 1}
        operands += before
    return pl.pallas_call(
        functools.partial(take_kernel, start),
        grid=(steps,),
        in_specs=in_specs,
        out_specs=[state_spec, state_spec],
        out_shape=[jax.ShapeDtypeStruct(memory.shape, kind) for kind in (f32, bf16)],
        input_output_aliases=aliases,
        compiler_params=pltpu.CompilerParams(vmem_limit_bytes=VMEM_LIMIT),
        cost_estimate=pl.CostEstimate(
            flops=memory.size * 64 // PIECES,
            bytes_accessed=memory.size * 8 // PIECES,
            transcendentals=0,
        ),
        name="take",
    )(*operands)


def finish_kernel(n_refs, position_ref, aux_ref, gain_ref, own_ref, right_ref, left_ref, *refs):
    state_ref, *refs = refs
    near_refs, far_refs, refs = refs[:n_refs], refs[n_refs : 2 * n_refs], refs[2 * n_refs :]
    away_ref, home_ref, acc, vectors, found_ref, flat, weights, sems = refs
    heads = state_ref.shape[1]
    step = pl.program_id(0)
    seqs = vectors.shape[2]
    rows = BLOCK * P_SIZE
    n_blocks = weights.shape[0]

    def each_copy(act):
        for k in range(n_refs):

            @pl.when(position_ref[k] >= 0)
            def _():
                for side, refs in enumerate((near_refs, far_refs)):
                    into = weights.at[position_ref[k], side]
                    act(pltpu.make_async_copy(refs[k], into, sems.at[k, side]))

    @pl.when(step == 0)
    def _():
        each_copy(lambda copy: copy.start())

    scale = aux_ref[pl.ds(step * rows, rows), :][:, 2 * heads : 2 * heads + 1]
    here = pl.ds(step * BLOCK, BLOCK)
    for kind in range(4):
        for h in range(heads):
            at = pl.ds((kind * heads + h) * DK, DK)
            total = own_ref[:, at] + right_ref[:, at].astype(f32) + left_ref[:, at].astype(f32)
            acc[kind * heads + h] = (total * scale).astype(bf16).astype(f32)
    for h in range(heads):
        picked = [
            acc[kind * heads + h, pl.ds(t, BLOCK, stride=P_SIZE), :]
            for kind in range(4)
            for t in range(P_SIZE)
        ]
        for n, value in enumerate(picked):
            vectors[n, h, here, :] = value
        outs = state_products(picked[: 2 * P_SIZE], state_ref, h)
        for n in range(2 * P_SIZE):
            found_ref[n, h, here, :] = rows_of(outs, n)

    @pl.when(step == pl.num_programs(0) - 1)
    def _():
        def whole(ref, n):
            return ref[n].reshape(heads * seqs, DK)

        def spread(table, first=0):
            return jnp.concatenate(
                [
                    jnp.broadcast_to(table[:, first + h : first + h + 1], (seqs, DK))
                    for h in range(heads)
                ],
                axis=0,
            )

        aux = [aux_ref[pl.ds(t, seqs, stride=P_SIZE), :] for t in range(P_SIZE)]
        starts, between = decay_tables(aux)
        gain = gain_ref[...]
        queries = [whole(vectors, t) for t in range(P_SIZE)]
        keys = [whole(vectors, P_SIZE + t) for t in range(P_SIZE)]
        norms = [lax.rsqrt(row_dot(k, k) + epsilon) for k in keys]
        writes = []
        for t in range(P_SIZE):
            start = spread(starts[t])
            steps = {i: spread(between[i, t]) for i in range(t)}
            value = whole(vectors, 2 * P_SIZE + t) - start * norms[t] * whole(found_ref, P_SIZE + t)
            for i in range(t):
                factor = steps[i] * (norms[i] * norms[t] * row_dot(keys[i], keys[t]))
                value = value - factor * writes[i]
            writes.append(spread(aux[t], heads) * value)
            query = queries[t]
            found = start * whole(found_ref, t)
            for i in range(t + 1):
                factor = norms[i] * row_dot(keys[i], query)
                if i < t:
                    factor = factor * steps[i]
                found = found + factor * writes[i]
            attended = found * (lax.rsqrt(row_dot(query, query) + epsilon) * DK ** (-0.5))
            mean = jnp.mean(attended * attended, axis=1, keepdims=True)
            gate = whole(vectors, 3 * P_SIZE + t)
            scaled = attended * lax.rsqrt(mean + epsilon) * gain * (gate * jax.nn.sigmoid(gate))
            for h in range(heads):
                flat[h, pl.ds(t, seqs, stride=P_SIZE), :] = scaled[h * seqs : (h + 1) * seqs]
        sides = heads // 2
        plane = position_ref[n_refs]
        lefts = [
            jnp.concatenate([flat[first + h] for h in range(sides)], axis=1).astype(bf16)
            for first in (plane * sides, (1 - plane) * sides)
        ]
        each_copy(lambda copy: copy.wait())
        cols = weights.shape[-1]
        for n in range(n_blocks):
            result = sum(
                jnp.dot(lefts[side], weights[n, side], preferred_element_type=f32)
                for side in range(2)
            ).astype(bf16)
            out_ref, at = (away_ref, n) if n < n_blocks // 2 else (home_ref, n - n_blocks // 2)
            out_ref[:, pl.ds(at * cols, cols)] = result


def finish(chunk, n_blocks, own, right, left, state, aux, gain, near, far, position):
    seqs, heads = state.shape[:2]
    rows = BLOCK * P_SIZE
    steps = seqs // BLOCK // ENDS
    start = chunk * steps
    first = start % (own.shape[0] // rows)
    n_refs = len(near)
    half, cols = near[0].shape
    part_spec = lambda at: pl.BlockSpec((rows, 4 * heads * DK), lambda i: (at + i, 0))
    out = jax.ShapeDtypeStruct((steps * rows, n_blocks // 2 * cols), bf16)
    out_spec = pl.BlockSpec(out.shape, lambda i: (0, 0))
    return pl.pallas_call(
        functools.partial(finish_kernel, n_refs),
        grid=(steps,),
        in_specs=[
            pl.BlockSpec(memory_space=pltpu.SMEM),
            pl.BlockSpec((steps * rows, 128), lambda i: (chunk, 0)),
            pl.BlockSpec((1, DK), lambda i: (0, 0)),
            part_spec(first),
            part_spec(0),
            part_spec(0),
            pl.BlockSpec((BLOCK, heads, DK, DK), lambda i: (start + i, 0, 0, 0)),
            *[pl.BlockSpec(memory_space=pl.ANY)] * (2 * n_refs),
        ],
        out_specs=[out_spec, out_spec],
        out_shape=[out, out],
        scratch_shapes=[
            pltpu.VMEM((4 * heads, rows, DK), f32),
            pltpu.VMEM((4 * P_SIZE, heads, steps * BLOCK, DK), f32),
            pltpu.VMEM((2 * P_SIZE, heads, steps * BLOCK, DK), f32),
            pltpu.VMEM((heads, steps * rows, DK), f32),
            pltpu.VMEM((n_blocks, 2, half, cols), bf16),
            pltpu.SemaphoreType.DMA((n_refs, 2)),
        ],
        compiler_params=pltpu.CompilerParams(vmem_limit_bytes=VMEM_LIMIT),
        cost_estimate=pl.CostEstimate(
            flops=state.size * 64 // ENDS,
            bytes_accessed=state.size * 2 // ENDS,
            transcendentals=0,
        ),
        name="finish",
    )(position, aux, gain, own, right, left, state, *near, *far)


def after(value, *others):
    return lax.optimization_barrier((value, *others))[0]


def on_device(
    sizes,
    candidate_embeddings,
    incoming_rms_scaling,
    probe_projector,
    address_projector,
    content_projector,
    sigmoid_mask_matrix,
    forgetting_projector,
    strength_projector_matrix,
    channel_forgetting_rates,
    forgetting_offset,
    extra_forgetting,
    outgoing_rms_scaling,
    final_projector,
    memory_matrix,
    earlier_addresses,
    earlier_contents,
    earlier_strengths,
    earlier_forgetting,
    admitted_counts,
):
    _, n_kv, n_tp = sizes
    rows, local_cols = candidate_embeddings.shape
    width = probe_projector.shape[1]
    heads = width // DK
    all_heads = forgetting_projector.shape[1]
    model = local_cols * n_tp
    per_tp = n_kv // n_tp
    kv_cols = model // n_kv
    z = lax.axis_index("kv")
    tp = lax.axis_index("tp")
    plane = lax.axis_index("grp")
    core = tp % CORES

    def swap(value, mask):
        return lax.ppermute(value, "tp", [(i, i ^ mask) for i in range(n_tp)])

    chunk_rows = rows // CHUNKS
    part_rows = chunk_rows // CORES

    gain_part = lax.dynamic_slice_in_dim(incoming_rms_scaling, tp * local_cols, local_cols)
    gained = (candidate_embeddings.astype(f32) * gain_part).astype(bf16)
    halves = []
    for chunk in range(CHUNKS):
        pieces = []
        for m in range(n_tp):
            at = chunk * chunk_rows + part_rows * ((tp ^ m) % CORES)
            pieces.append(lax.dynamic_slice_in_dim(gained, at, part_rows))
        for m in range(n_tp - 1, 0, -1):
            pieces[m] = swap(pieces[m], m)
        halves.append(jnp.stack(pieces))

    half = width // 2
    near = lax.dynamic_slice_in_dim(final_projector, plane * half, half)
    far = lax.dynamic_slice_in_dim(final_projector, (1 - plane) * half, half)
    rights, lefts = [near], [near]
    far_rights, far_lefts = [far], [far]

    def weight_round(i, *others):
        right, left = lax.optimization_barrier((rights[-1], lefts[-1], *others))[:2]
        pairs = [(j, j + 1) for j in range(i - 1, n_kv - 1)]
        rights.append(lax.ppermute(right, "kv", pairs))
        pairs = [(j + 1, j) for j in range(0, n_kv - i)]
        lefts.append(lax.ppermute(left, "kv", pairs))

    def weight_cross(i):
        def pairs(places):
            return [(g * n_kv + j, (1 - g) * n_kv + j) for g in range(2) for j in places]

        both = ("grp", "kv")
        right, left = lax.optimization_barrier((rights[i], lefts[i]))
        far_rights.append(lax.ppermute(right, both, pairs(range(i, n_kv))))
        far_lefts.append(lax.ppermute(left, both, pairs(range(n_kv - i))))

    weight_round(1, gained)

    joined = jnp.concatenate(
        [probe_projector, address_projector, content_projector, sigmoid_mask_matrix], axis=1
    )

    received = []
    for chunk in range(CHUNKS):

        def block_for(dest):
            return lax.dynamic_slice(
                halves[chunk],
                (tp ^ (dest // per_tp), 0, (dest % per_tp) * kv_cols),
                (1, part_rows, kv_cols),
            )[0]

        sends = [block_for((z + k) % n_kv) for k in range(n_kv)]
        *sends, joined = lax.optimization_barrier((*sends, joined))
        received.append(
            [sends[0]]
            + [
                lax.ppermute(sends[k], "kv", [(i, (i + k) % n_kv) for i in range(n_kv)])
                for k in range(1, n_kv)
            ]
        )

    blocks = [None] * CHUNKS
    products = [{} for _ in range(CHUNKS)]
    arrived = [None] * CHUNKS
    token = received[0][0]
    crossing = crossing_order(n_kv)
    for i in range(1, n_kv):
        for chunk in range(CHUNKS):
            product = products[chunk]
            if i == 1:
                mine = lax.optimization_barrier((*received[chunk], token))[:n_kv]
                blocks[chunk] = [None] * n_kv
                for k in crossing:
                    partner = swap(mine[k], 1)
                    blocks[chunk][k] = jnp.concatenate(
                        [
                            jnp.where(core == 0, mine[k], partner),
                            jnp.where(core == 0, partner, mine[k]),
                        ]
                    )
            if i <= n_kv // 2:
                pair = [i, n_kv - i] if i < n_kv - i else [0, i]
                block = jnp.concatenate([blocks[chunk][k] for k in pair], axis=0)
                block = after(block, token)
                out = jnp.dot(block, joined, preferred_element_type=f32)
                out = lax.optimization_barrier(out)
                for n, k in enumerate(pair):
                    product[k] = out[n * chunk_rows : (n + 1) * chunk_rows]
            sends = [product[i], product[n_kv - i]]
            places = (
                [(j, j + 1) for j in range(i)],
                [(j, j - 1) for j in range(n_kv - i, n_kv)],
            )
            parts = ENDS // CHUNKS if i == n_kv - 1 else 1
            part = chunk_rows // parts
            for side in range(2):
                if arrived[chunk] is not None:
                    there = after(arrived[chunk][0][side], token)
                    sends[side] = sends[side] + there.astype(f32)
                token = sends[side] = lax.optimization_barrier(sends[side].astype(bf16))
            got = []
            for n in range(parts):
                both = []
                for side in range(2):
                    send = sends[side]
                    if parts > 1:
                        send = lax.optimization_barrier(send[n * part : (n + 1) * part])
                    both.append(lax.ppermute(send, "kv", places[side]))
                got.append(tuple(both))
            arrived[chunk] = got
            if chunk == 0:
                if i + 1 < n_kv:
                    weight_round(i + 1, token)
                weight_cross(i)

    early = lax.optimization_barrier(
        (
            admitted_counts,
            earlier_forgetting,
            earlier_strengths,
            earlier_addresses,
            earlier_contents,
            gained,
        )
    )
    live = early[0][:, None, None] > jnp.arange(P_SIZE)[None, :, None]
    early_decay = jnp.where(live, early[1], 0.0)
    early_aux = jnp.concatenate([early_decay, jnp.where(live, early[2], 0.0)], axis=2)
    early_aux = jnp.pad(early_aux.reshape(rows, 2 * heads), ((0, 0), (0, 128 - 2 * heads)))
    by_head = lambda values: jnp.transpose(values, (1, 2, 0, 3)).astype(f32)
    early_keys, early_values = by_head(early[3]), by_head(early[4])
    early_last = jnp.exp(jnp.sum(early_decay, axis=1))
    taken = None
    for piece in range(PIECES):
        taken = take(piece, taken, memory_matrix, early_keys, early_values, early_aux, early_last)

    small = jnp.concatenate([forgetting_projector, strength_projector_matrix], axis=1)
    small = lax.dynamic_slice_in_dim(small, tp * local_cols, local_cols)
    raw = candidate_embeddings.astype(f32)
    sums = jnp.concatenate(
        [
            jnp.dot(gained, small, preferred_element_type=f32),
            jnp.sum(raw * raw, axis=1, keepdims=True),
        ],
        axis=1,
    )
    mask = 1
    while mask < n_tp:
        sums = sums + swap(sums, mask)
        mask *= 2
    scale = lax.rsqrt(sums[:, 2 * all_heads :] / model + epsilon)
    own = lambda at: lax.dynamic_slice_in_dim(sums, at + tp * heads, heads, 1) * scale
    log_decay = -jnp.exp(channel_forgetting_rates) * jax.nn.softplus(
        own(0) + forgetting_offset
    ) + extra_forgetting.reshape(rows, heads)
    aux = jnp.concatenate([log_decay, jax.nn.sigmoid(own(all_heads)), scale], axis=1)
    aux = jnp.pad(aux, ((0, 0), (0, 128 - aux.shape[1])))
    gain = outgoing_rms_scaling[None]

    offsets = [0] + [-i for i in range(1, n_kv)] + list(range(1, n_kv))
    source = z + jnp.array(offsets, dtype=jnp.int32)
    apart = tp ^ (source // per_tp)
    position = (apart // 2 + jnp.where(apart % 2 == 0, n_tp // 2, 0)) * per_tp + source % per_tp
    position = jnp.where((source >= 0) & (source < n_kv), position, -1)
    position = jnp.concatenate([position, plane[None]]).astype(jnp.int32)
    results = []
    for end in range(ENDS):
        chunk = end * CHUNKS // ENDS
        away, home = finish(
            end,
            n_kv,
            products[chunk][0],
            *arrived[chunk][end % (ENDS // CHUNKS)],
            taken[1],
            aux,
            gain,
            rights + lefts[1:],
            far_rights + far_lefts[1:],
            position,
        )
        home = home.astype(f32) + swap(away, 1).astype(f32)
        result = home[:, :local_cols]
        for m in range(1, n_tp // 2):
            piece = home[:, m * local_cols : (m + 1) * local_cols].astype(bf16)
            result = result + swap(piece, 2 * m).astype(f32)
        results.append(result.astype(bf16))
    return (jnp.concatenate(results, axis=0), taken[0])


def crossing_order(n_kv):
    first = [k for i in range(1, (n_kv + 1) // 2) for k in (i, n_kv - i)]
    return first + [k for k in range(n_kv) if k not in first]


def solution(mesh):
    in_specs = (
        P(("grp", "kv"), "tp"),
        P(),
        P("kv", "tp"),
        P("kv", "tp"),
        P("kv", "tp"),
        P("kv", "tp"),
        P(),
        P(),
        P("tp"),
        P("tp"),
        P(("grp", "kv"), None, "tp"),
        P(),
        P("tp", "kv"),
        P(("grp", "kv"), "tp", None, None),
        P(("grp", "kv"), None, "tp", None),
        P(("grp", "kv"), None, "tp", None),
        P(("grp", "kv"), None, "tp"),
        P(("grp", "kv"), None, "tp"),
        P(("grp", "kv")),
    )
    out_specs = (P(("grp", "kv"), "tp"), P(("grp", "kv"), "tp", None, None))
    sizes = tuple(mesh.shape[name] for name in ("grp", "kv", "tp"))

    def layer(*arrays):
        return on_device(sizes, *arrays)

    return jax.shard_map(
        layer, mesh=mesh, in_specs=in_specs, out_specs=out_specs, check_vma=False
    )
```
